32 devices in a mesh: sp: 8 (over z, x), tp: 4 (over y, core).
Axes of the slice: x: 2, y: 2, z: 4, core: 2. Of those that a mesh axis runs over, the one named last changes fastest.
Arguments:
- moe_input: bfloat16 [1536, 2048], P('sp'), may hold values from -6 to 6
- out_grad: bfloat16 [1536, 2048], P('sp', 'tp'), may hold values from -6 to 6
- expert_ids: int32 [1536, 2], P('sp'), may hold values from 0 to 7, all different within a row; in each aligned block of 192 rows (0 to 191, 192 to 383, ...) at most 60 rows name the same one
- expert_weights: float32 [1536, 2], P('sp'), may hold values from 0.1 to 0.9
- w_gate: bfloat16 [8, 2048, 2048], P('sp', None, 'tp'), may hold values from -0.125 to 0.125
- w_up: bfloat16 [8, 2048, 2048], P('sp', None, 'tp'), may hold values from -0.125 to 0.125
- w_down: bfloat16 [8, 2048, 2048], P('sp', 'tp'), may hold values from -0.125 to 0.125
- out_proj: bfloat16 [1536, 2048], P('tp'), may hold values from -0.15625 to 0.15625
- retained: bfloat16 [1536, 1536], P('sp', 'tp'), may hold values from -6 to 6
- queries: bfloat16 [1536, 768], P('sp', 'tp'), may hold values from -6 to 6
- keys: bfloat16 [1536, 768], P('sp', 'tp'), may hold values from -0.86328125 to 0.86328125
- values: bfloat16 [1536, 1536], P('sp', 'tp'), may hold values from -6 to 6
- log_decay: float32 [1536, 16], P('sp', 'tp'), may hold values from -1 to 0
- incoming_state: float32 [8, 16, 48, 96], P('sp', 'tp'), may hold values from -6 to 6
Outputs:
- w_gate_grad: bfloat16 [8, 2048, 2048], P('sp', None, 'tp')
- w_up_grad: bfloat16 [8, 2048, 2048], P('sp', None, 'tp')
- w_down_grad: bfloat16 [8, 2048, 2048], P('sp', 'tp')
- out_proj_grad: float32 [2048, 1536], P('sp', 'tp')
- query_grad: bfloat16 [1536, 768], P('sp', 'tp')
- key_grad: bfloat16 [1536, 768], P('sp', 'tp')
- value_grad: bfloat16 [1536, 1536], P('sp', 'tp')
The draws below stay inside these ranges and needn't reach their ends.
Inputs may be any that keep to these rules, and one draw needn't show every extreme that they name: `expert_ids`: in each aligned block of 192 positions no expert is named by more than 60 of the block's assignments, a bound that some block reaches.
All inputs are finite; a program needn't handle non-finite values.
Results may differ from the reference program's by a relative error of at most 0.02.
Values may be sent and summed in bfloat16 or wider, within the bound.
No kernel may reach another device: no remote copies, remote signals or barrier semaphores. Data moves between devices by JAX's collectives and lax.ppermute only.
A program may use at most 64 MiB of HBM per device.

```python
import math
import jax
import jax.numpy as jnp
import numpy as np
from jax import lax

D = 2048
RETENTION_HEADS = 16
KEY_DIM = 48
VALUE_DIM = 96
FF = 2048
TOK_DEV = 192
SEQUENCE_TOKENS = 1536
EXPERTS = 8
CAP = 60
RET_WIDTH = 1536
KEY_WIDTH = 768
N_SP = 8
N_TP = 4


def draw_log_decay(key, part):
    keys = jax.random.split(jax.random.fold_in(key, 17), 7)
    slow_share = 0.5
    slow = jax.random.uniform(keys[0], (RETENTION_HEADS,), jnp.float32) < slow_share
    slow_rate = jnp.exp(jax.random.uniform(keys[1], (RETENTION_HEADS,), jnp.float32, jnp.log(0.1), jnp.log(0.6))) / SEQUENCE_TOKENS
    fast_rate = jax.random.uniform(keys[2], (RETENTION_HEADS,), jnp.float32, 1.0 / 50.0, 1.0 / 30.0)
    decay_rate = jnp.where(slow, slow_rate, fast_rate)
    block_multiplier = jnp.repeat(jax.random.uniform(keys[3], (SEQUENCE_TOKENS // TOK_DEV,), jnp.float32, 0.5, 1.6), TOK_DEV)
    coarse_estimate = jax.random.uniform(keys[4], (SEQUENCE_TOKENS, 1), jnp.float32, 0.5, 1.5)
    spike_position = jax.random.randint(keys[5], (3,), 0, SEQUENCE_TOKENS)
    spike_mask = jnp.any(jnp.arange(SEQUENCE_TOKENS)[:, None] == spike_position[None, :], axis=1).astype(jnp.float32)
    spike_length = jax.random.uniform(keys[6], (RETENTION_HEADS,), jnp.float32, 0.22, 0.51)
    return -(decay_rate[None, :] * block_multiplier[:, None] * coarse_estimate) - spike_mask[:, None] * spike_length[None, :]


def raised(drawn, rng, source, target, blocks, factor):
    owner, partner = [(jnp.arange(drawn.shape[axis_at]) // (drawn.shape[axis_at] // blocks)).reshape([-1 if axis == axis_at else 1 for axis in range(drawn.ndim)]) for axis_at in (source, target)]
    chosen = jax.random.permutation(rng, blocks)[partner]
    strong = (owner == chosen) | (owner == (partner + blocks // 2) % blocks)
    return jnp.where(strong, factor * drawn, drawn)


def block_scale(key, shape, pieces, smallest, high):
    def one(position, blocks):
        heights = jax.random.uniform(jax.random.fold_in(jax.random.fold_in(key, 6), position), (blocks,), jnp.float32, smallest / len(pieces), high / len(pieces))
        return jnp.repeat(jnp.exp(heights), shape[position] // blocks).reshape((-1,) + (1,) * (len(shape) - position - 1))

    gain = one(*pieces[0])
    for cut in pieces[1:]:
        gain = gain * one(*cut)
    return gain


def deal_out(rng, own, number, rows, number_of, top, bound, slope):
    sequence = jax.random.permutation(rng, number_of)
    crowded, usual = load_shares(number_of, rows * top, bound, slope, True), load_shares(number_of, rows * top, bound, slope, False)
    places = jnp.arange(number_of)

    def named(tallies, rotation):
        used = int((tallies > 0).sum())
        fixed = max(1, used // 4)
        moved = fixed + (places - fixed + rotation * (used - fixed)) % max(1, number_of - fixed)
        return jnp.zeros((number_of,), jnp.int32).at[sequence[jnp.where(places < fixed, places, moved)]].set(jnp.asarray(tallies, jnp.int32))

    tallies = jnp.where(number % 4 == 0, named(crowded, number // 4), named(usual, number - number // 4 - 1))
    mixed = jax.random.permutation(jax.random.fold_in(own, 3), number_of)
    giver, receiver = mixed[0:number_of // 2 * 2:2], mixed[1:number_of // 2 * 2:2]
    slack = jnp.minimum(tallies[giver] - 1, bound - tallies[receiver]) // 2
    slack = jnp.where((giver == sequence[0]) | (receiver == sequence[0]) | (tallies[receiver] == 0), 0, jnp.maximum(slack, 0))
    moved = jax.random.randint(jax.random.fold_in(own, 4), (number_of // 2,), 0, 1 << 20) % (slack + 1)
    tallies = tallies.at[giver].add(-moved).at[receiver].add(moved)
    items = jnp.searchsorted(jnp.cumsum(tallies), jnp.arange(rows * top), side="right").astype(jnp.int32)
    grid = items.reshape(top, rows).T
    grid = grid[jax.random.permutation(jax.random.fold_in(own, 1), rows)]
    rotation = jax.random.randint(jax.random.fold_in(own, 2), (rows, 1), 0, top)
    return jnp.take_along_axis(grid, (jnp.arange(top)[None, :] + rotation) % top, axis=1)


def load_shares(number_of, total, reach, lean, full):
    loads = [(1 << 20) // math.isqrt(grade ** lean) + 1 for grade in range(1, number_of + 1)]
    largest = reach if full else min(reach, max(-(-total // number_of), total * loads[0] // sum(loads)))
    least = 1 if total - largest >= number_of - 1 else 0
    given, spare = [largest] + [least] * (number_of - 1), total - largest - least * (number_of - 1)
    while spare > 0:
        free = [i for i in range(1, number_of) if given[i] < largest] or [i for i in range(1, number_of) if given[i] < reach]
        pool, left = sum([loads[i] for i in free]), spare
        for i in free:
            addition = min(reach - given[i], max(1, left * loads[i] // pool), spare)
            given[i] = given[i] + addition
            spare = spare - addition
    return np.array(given)


def normal_values(key, dims, deviation, bound, cuts=(), kind=jnp.bfloat16):
    drawn = deviation * jax.random.normal(key, dims, jnp.float32)
    if cuts:
        drawn = drawn * block_scale(key, dims, cuts, -0.22, 0.18)
    return jnp.clip(drawn, -bound, bound).astype(kind)


def gaussian_with(key, shape, deviation, reach, cuts, heavy, kind=jnp.bfloat16):
    drawn = deviation * jax.random.normal(key, shape, jnp.float32)
    if cuts:
        drawn = drawn * block_scale(key, shape, cuts, -0.22, 0.18)
    return jnp.clip(raised(drawn, jax.random.fold_in(key, 3), *heavy), -reach, reach).astype(kind)


def setup_inputs(seed: int = 0) -> dict:
    key_list = jax.random.split(jax.random.key(seed), 15)
    moe_input = normal_values(key_list[0], (SEQUENCE_TOKENS, D), 1.0, 6.0, ((0, 8),))
    out_grad = gaussian_with(key_list[1], (SEQUENCE_TOKENS, D), 1.0, 6.0, ((0, 8), (1, 4)), (0, 1, 8, 2.0))
    expert_ids_keys = jax.random.split(jax.random.fold_in(key_list[2], 1), SEQUENCE_TOKENS // TOK_DEV)
    expert_ids_turns = jax.random.permutation(jax.random.fold_in(key_list[2], 3), SEQUENCE_TOKENS // TOK_DEV)
    expert_ids = jax.vmap(lambda own, number: deal_out(jax.random.fold_in(key_list[2], 2), own, number, TOK_DEV, EXPERTS, 2, CAP, 1))(expert_ids_keys, expert_ids_turns).reshape((SEQUENCE_TOKENS, 2))
    expert_weights = jnp.clip(0.1 + 0.79999997 * jax.random.uniform(key_list[3], (SEQUENCE_TOKENS, 2), jnp.float32) ** block_scale(key_list[3], (SEQUENCE_TOKENS, 2), ((0, 8),), -0.2, 0.2), 0.1, 0.9)
    w_gate = normal_values(key_list[4], (EXPERTS, D, FF), D ** -0.5, 0.125, ((0, 8), (2, 4)))
    w_up = normal_values(key_list[5], (EXPERTS, D, FF), D ** -0.5, 0.125, ((0, 8), (2, 4)))
    w_down = normal_values(key_list[6], (EXPERTS, FF, D), FF ** -0.5, 0.125, ((0, 8), (1, 4)))
    out_proj = normal_values(key_list[7], (RET_WIDTH, D), RET_WIDTH ** -0.5, 0.15625, ((0, 4),))
    retained = normal_values(key_list[8], (SEQUENCE_TOKENS, RET_WIDTH), 1.0, 6.0, ((0, 8), (1, 4)))
    queries = normal_values(key_list[9], (SEQUENCE_TOKENS, KEY_WIDTH), 1.0, 6.0, ((0, 8), (1, 4)))
    keys = normal_values(key_list[10], (SEQUENCE_TOKENS, KEY_WIDTH), (KEY_DIM ** -0.5), 0.86328125, ((0, 8), (1, 4)))
    values = normal_values(key_list[11], (SEQUENCE_TOKENS, RET_WIDTH), 1.0, 6.0, ((0, 8), (1, 4)))
    log_decay = draw_log_decay(jax.random.fold_in(key_list[14], 71), 0)
    incoming_state = normal_values(key_list[13], (N_SP, RETENTION_HEADS, KEY_DIM, VALUE_DIM), 1.0, 6.0, ((0, 8), (1, 4)), jnp.float32)
    return dict(moe_input=moe_input, out_grad=out_grad, expert_ids=expert_ids, expert_weights=expert_weights, w_gate=w_gate, w_up=w_up, w_down=w_down, out_proj=out_proj, retained=retained, queries=queries, keys=keys, values=values, log_decay=log_decay, incoming_state=incoming_state)


def slot_table(expert_ids, expert_weights):
    per_block = expert_ids.reshape(N_SP, 2 * TOK_DEV)
    block_weights = expert_weights.reshape(N_SP, 2 * TOK_DEV)
    onehot = (per_block[:, :, None] == jnp.arange(EXPERTS, dtype=jnp.int32)[None, None, :]).astype(jnp.int32)
    ranks = jnp.sum((jnp.cumsum(onehot, axis=1) - onehot) * onehot, axis=2).astype(jnp.int32)
    block = jnp.arange(N_SP, dtype=jnp.int32)[:, None]
    dest = (per_block * (N_SP * CAP) + block * CAP + ranks).reshape(-1).astype(jnp.int32)
    token = (block * TOK_DEV + jnp.arange(2 * TOK_DEV, dtype=jnp.int32)[None, :] // 2).reshape(-1).astype(jnp.int32)
    table = jnp.full((EXPERTS * N_SP * CAP,), SEQUENCE_TOKENS, jnp.int32).at[dest].set(token)
    weight = jnp.zeros((EXPERTS * N_SP * CAP,), jnp.float32).at[dest].set(block_weights.reshape(-1))
    return table.reshape(EXPERTS, N_SP * CAP), weight.reshape(EXPERTS, N_SP * CAP)


def reference(moe_input, out_grad, expert_ids, expert_weights, w_gate, w_up, w_down, out_proj,
              retained, queries, keys, values, log_decay, incoming_state):
    f32 = jnp.float32
    bf16 = jnp.bfloat16
    upper_limit = lax.Precision.HIGHEST
    table, weight = slot_table(expert_ids, expert_weights)
    padded_rows = jnp.concatenate([moe_input, jnp.zeros((1, D), bf16)], axis=0)
    padded_grad = jnp.concatenate([out_grad, jnp.zeros((1, D), bf16)], axis=0)
    part = FF // N_TP

    def expert_back(args):
        index, slot_weight, gate_w, up_w, down_w = args
        rows = padded_rows[index]
        grad = (padded_grad[index].astype(f32) * slot_weight[:, None]).astype(bf16)
        gate = jnp.dot(rows, gate_w, preferred_element_type=f32)
        up = jnp.dot(rows, up_w, preferred_element_type=f32)
        sig = jax.nn.sigmoid(gate)
        swish = gate * sig
        act = (swish * up).astype(bf16)
        act_grad = jnp.dot(grad, down_w.T, preferred_element_type=f32)
        gate_grad = (act_grad * up * sig * (1.0 + gate * (1.0 - sig))).astype(bf16)
        up_grad = (act_grad * swish).astype(bf16)
        down_grad = jnp.dot(act.T, grad, preferred_element_type=f32).astype(bf16)
        gate_w_grad = jnp.dot(rows.T, gate_grad, preferred_element_type=f32).astype(bf16)
        up_w_grad = jnp.dot(rows.T, up_grad, preferred_element_type=f32).astype(bf16)
        slots = rows.shape[0]
        parts = (jnp.einsum('snf,dnf->nsd', gate_grad.astype(f32).reshape(slots, N_TP, part),
                            gate_w.astype(f32).reshape(D, N_TP, part))
                 + jnp.einsum('snf,dnf->nsd', up_grad.astype(f32).reshape(slots, N_TP, part),
                              up_w.astype(f32).reshape(D, N_TP, part)))
        rounded = lax.optimization_barrier(parts.astype(bf16))
        slot_in = jnp.sum(rounded.astype(f32), axis=0).astype(bf16)
        return gate_w_grad, up_w_grad, down_grad, slot_in

    w_gate_grad, w_up_grad, w_down_grad, slot_in = lax.map(expert_back, (table, weight, w_gate, w_up, w_down))
    token_grad = jnp.zeros((SEQUENCE_TOKENS + 1, D), f32).at[table.reshape(-1)].add(
        slot_in.reshape(-1, D).astype(f32))[:SEQUENCE_TOKENS]
    stream = (out_grad.astype(f32) + token_grad).astype(bf16)
    ret_grad = jnp.dot(stream, out_proj.T, preferred_element_type=f32).astype(bf16)
    out_proj_grad = jnp.dot(stream.T, retained, preferred_element_type=f32)

    q = queries.astype(f32).reshape(N_SP, TOK_DEV, RETENTION_HEADS, KEY_DIM)
    k = keys.astype(f32).reshape(N_SP, TOK_DEV, RETENTION_HEADS, KEY_DIM)
    v = values.astype(f32).reshape(N_SP, TOK_DEV, RETENTION_HEADS, VALUE_DIM)
    o = ret_grad.astype(f32).reshape(N_SP, TOK_DEV, RETENTION_HEADS, VALUE_DIM)
    b = jnp.cumsum(log_decay.reshape(N_SP, TOK_DEV, RETENTION_HEADS), axis=1)
    b_end = b[:, -1]
    diff = b[:, :, None, :] - b[:, None, :, :]
    place = jnp.arange(TOK_DEV)
    causal = (place[:, None] >= place[None, :])[None, :, :, None]
    decay = jnp.where(causal, jnp.exp(jnp.minimum(diff, 0.0)), 0.0)
    scores = jnp.einsum('nthk,nshk->ntsh', q, k, precision=upper_limit) * decay
    prob_grad = jnp.einsum('nthv,nshv->ntsh', o, v, precision=upper_limit) * decay
    added_input = jnp.einsum('nth,nthk,nthv->nhkv', jnp.exp(b), q, o, precision=upper_limit)

    def back_step(carry, inputs):
        factor, term = inputs
        return term + factor[:, None, None] * carry, carry

    _, state_gradient = lax.scan(back_step, jnp.zeros((RETENTION_HEADS, KEY_DIM, VALUE_DIM), f32),
                             (jnp.exp(b_end), added_input), reverse=True)
    tail = jnp.exp(b_end[:, None, :] - b)[..., None]
    query_grad = (jnp.einsum('ntsh,nshk->nthk', prob_grad, k, precision=upper_limit)
                  + jnp.exp(b)[..., None] * jnp.einsum('nthv,nhkv->nthk', o, incoming_state, precision=upper_limit))
    key_grad = (jnp.einsum('ntsh,nthk->nshk', prob_grad, q, precision=upper_limit)
                + tail * jnp.einsum('nshv,nhkv->nshk', v, state_gradient, precision=upper_limit))
    value_grad = (jnp.einsum('ntsh,nthv->nshv', scores, o, precision=upper_limit)
                  + tail * jnp.einsum('nshk,nhkv->nshv', k, state_gradient, precision=upper_limit))
    return (w_gate_grad, w_up_grad, w_down_grad, out_proj_grad,
            query_grad.reshape(SEQUENCE_TOKENS, KEY_WIDTH).astype(bf16),
            key_grad.reshape(SEQUENCE_TOKENS, KEY_WIDTH).astype(bf16),
            value_grad.reshape(SEQUENCE_TOKENS, RET_WIDTH).astype(bf16))
```

```python
import functools

import jax
import jax.numpy as jnp
from jax import lax
from jax.experimental import pallas as pl
from jax.experimental.pallas import tpu as pltpu
from jax.sharding import PartitionSpec as P


F32 = jnp.float32
BF16 = jnp.bfloat16
ACROSS = (((1,), (1,)), ((), ()))
ALONG = (((0,), (0,)), ((), ()))
CHUNKS = 2
START_VMEM = 60 << 20
WEIGHTS_VMEM = 52 << 20


def swap(x, axis, offset):
    count = lax.axis_size(axis)
    return lax.ppermute(x, axis, [(d, d ^ offset) for d in range(count)])


def powers(count):
    bits = []
    bit = 1
    while bit < count:
        bits.append(bit)
        bit *= 2
    return bits


def dot(a, b, dims=(((1,), (0,)), ((), ()))):
    return lax.dot_general(a, b, dims, preferred_element_type=F32)


def lanes(shape, head, per_head):
    lane = lax.broadcasted_iota(jnp.int32, shape, 1)
    return (lane >= head * per_head) & (lane < (head + 1) * per_head)


def spread_heads(columns, shape, per_head):
    out = jnp.zeros(shape, F32)
    for head in range(shape[1] // per_head):
        out = jnp.where(lanes(shape, head, per_head), columns[:, head : head + 1], out)
    return out


def masked(x, head, per_head):
    return jnp.where(lanes(x.shape, head, per_head), x, jnp.zeros_like(x))


def blocks_on_diagonal(packed, heads, value_dim):
    return jnp.concatenate([masked(packed, head, value_dim) for head in range(heads)], axis=0)


def start_kernel(tp_ref, sp_ref, *refs, slots, blocks, heads, key_dim, value_dim):
    sources, outs, scratch, arrivals = refs[:9], refs[9 : 17 + blocks], refs[17 + blocks : -1], refs[-1]
    send_refs, outs = outs[:blocks], outs[blocks:]
    columns = scratch[3].shape[1]
    start = pl.multiple_of(tp_ref[0] * columns, 128)
    copies = [
        pltpu.make_async_copy(
            source.at[:, pl.ds(start, columns)] if n == 2 else source, target, arrivals.at[n]
        )
        for n, (source, target) in enumerate(zip(sources, scratch))
    ]
    for copy in copies:
        copy.start()
    pick_part(copies, sp_ref, *scratch[:4], send_refs, outs[0], slots=slots, blocks=blocks)
    for copy in copies[4:]:
        copy.wait()
    prepare_part(*scratch[4:], *outs[1:], heads=heads, key_dim=key_dim, value_dim=value_dim)


def pick_part(copies, sp_ref, ids_ref, weights_ref, rows_ref, grad_ref, send_refs, pick_ref, *, slots, blocks):
    columns = grad_ref.shape[1]
    copies[0].wait()
    tokens = ids_ref.shape[1]
    total = slots * blocks
    first, second = ids_ref[0:1, :], ids_ref[1:2, :]
    expert = lax.broadcasted_iota(jnp.int32, (-(-blocks // 16) * 16, tokens), 0)
    one, two = expert == first, expert == second
    both = jnp.where(one | two, 1.0, 0.0).astype(BF16)
    row = lax.broadcasted_iota(jnp.int32, (tokens, tokens), 0)
    col = lax.broadcasted_iota(jnp.int32, (tokens, tokens), 1)
    count = dot(both, jnp.where(row < col, 1.0, 0.0).astype(BF16))
    rank_one = jnp.sum(jnp.where(one, count, 0.0), axis=0, keepdims=True)
    rank_two = jnp.sum(jnp.where(two, count, 0.0), axis=0, keepdims=True)

    slot_one = (first ^ sp_ref[0]) * slots + rank_one.astype(jnp.int32)
    slot_two = (second ^ sp_ref[0]) * slots + rank_two.astype(jnp.int32)
    position = lax.broadcasted_iota(jnp.int32, (total, tokens), 0)
    hit_one, hit_two = position == slot_one, position == slot_two
    pick = jnp.where(hit_one | hit_two, 1.0, 0.0).astype(BF16)
    copies[1].wait()
    weight = jnp.sum(
        jnp.where(hit_one, weights_ref[0:1, :], 0.0) + jnp.where(hit_two, weights_ref[1:2, :], 0.0),
        axis=1,
        keepdims=True,
    )
    copies[2].wait()
    rows = dot(pick, rows_ref[...]).astype(BF16)
    copies[3].wait()
    grad = (dot(pick, grad_ref[...]) * weight).astype(BF16)
    for k in range(blocks):
        send_refs[k][:, :columns] = rows[k * slots : (k + 1) * slots]
        send_refs[k][:, columns:] = grad[k * slots : (k + 1) * slots]
    diagonal = row == col

    def as_column(line):
        return jnp.sum(jnp.where(diagonal, line, jnp.zeros_like(line)), axis=1, keepdims=True)

    place = lax.broadcasted_iota(jnp.int32, (tokens, total), 1)
    found = (place == as_column(slot_one)) | (place == as_column(slot_two))
    pick_ref[...] = jnp.where(found, 1.0, 0.0).astype(BF16)


def three_terms(x):
    high = x.astype(BF16)
    rest = x - high.astype(F32)
    middle = rest.astype(BF16)
    return high, middle, (rest - middle.astype(F32)).astype(BF16)


def prepare_part(log_ref, q_ref, k_ref, state_ref, kept_ref, decay_ref, decay_t_ref, scores_t_ref, qe_ref, sum_ref, incoming_ref, wide_ref, *, heads, key_dim, value_dim):
    tokens = q_ref.shape[0]
    row = lax.broadcasted_iota(jnp.int32, (tokens, tokens), 0)
    col = lax.broadcasted_iota(jnp.int32, (tokens, tokens), 1)
    below = jnp.where(col <= row, 1.0, 0.0).astype(BF16)
    terms = three_terms(log_ref[...])
    sums = sum([dot(below, term, ACROSS) for term in terms])
    flats = sum([dot(term, below, ACROSS) for term in terms])
    sum_ref[...] = sums[:, :heads]
    q, k = q_ref[...], k_ref[...]
    for head in range(heads):
        down = sums[:, head : head + 1]
        flat = flats[head : head + 1, :]
        decay = jnp.where(row >= col, jnp.exp(jnp.minimum(down - flat, 0.0)), 0.0)
        decay_t = jnp.where(col >= row, jnp.exp(jnp.minimum(flat - down, 0.0)), 0.0)
        decay_ref[head] = decay
        decay_t_ref[head] = decay_t
        scores_t_ref[head] = (dot(masked(k, head, key_dim), q, ACROSS) * decay_t).astype(BF16)
    qe_ref[...] = (q.astype(F32) * spread_heads(jnp.exp(sums), q.shape, key_dim)).astype(BF16)
    width = heads * value_dim
    from_lane = lax.broadcasted_iota(jnp.int32, (value_dim, width), 0)
    to_lane = lax.broadcasted_iota(jnp.int32, (value_dim, width), 1)
    for head in range(heads):
        put = jnp.where(to_lane == from_lane + head * value_dim, 1.0, 0.0).astype(BF16)
        incoming_ref[head * key_dim : (head + 1) * key_dim, :] = dot(
            state_ref[head].astype(BF16), put
        ).astype(BF16)
    last = spread_heads(sums[tokens - 8 : tokens], (8, width), value_dim)[7:8]
    high, middle, low = three_terms(last)
    line = lax.broadcasted_iota(jnp.int32, (16, width), 0)
    extra = jnp.where(line == 0, high.astype(F32), 0.0)
    extra = jnp.where(line == 1, middle.astype(F32), extra)
    extra = jnp.where(line == 2, low.astype(F32), extra)
    extra = extra.astype(BF16)
    kept = kept_ref[...]
    for block in range(wide_ref.shape[0]):
        wide_ref[block, :tokens, :] = kept
        wide_ref[block, tokens:, :] = extra


def order_kernel(tp_ref, sp_ref, wide_ref, last_ref, own_ref, other_ref, sums_ref, *, turn):
    kept, rows, _ = wide_ref.shape
    half = (rows - 16) // 2
    own = pl.multiple_of((tp_ref[0] & 1) * half, 16)
    for position in range(2 * kept):
        offset = sum(bit for step, bit in enumerate(turn) if position >> step & 1)
        ref, at = (wide_ref, position) if position < kept else (last_ref, position - kept)
        block = sp_ref[0] ^ offset
        target = pl.ds(pl.multiple_of(block * half, 16), half)
        own_ref[target, :] = ref[at, pl.ds(own, half), :]
        other_ref[target, :] = ref[at, pl.ds(half - own, half), :]
        tail = ref[at, 2 * half :, :].astype(F32)
        sums_ref[pl.ds(block, 1), :] = tail[0:1] + tail[1:2] + tail[2:3]


def pair_kernel(sp_ref, sums_ref, added_ref, partner_ref, pair_ref):
    odd = (sp_ref[0] & 1) == 1
    added, partner = added_ref[...].astype(F32), partner_ref[...].astype(F32)
    first, second = jnp.where(odd, partner, added), jnp.where(odd, added, partner)
    decay = jnp.exp(sums_ref[pl.ds(sp_ref[0] & ~1, 1), :])
    pair_ref[...] = (first + decay * second).astype(BF16)


def inject_kernel(stream_ref, proj_ref, qe_ref, o_ref, inject_ref, *, heads, key_dim, value_dim):
    o = dot(stream_ref[...], proj_ref[...], ACROSS).astype(BF16)
    o_ref[...] = o
    cross = dot(qe_ref[...], o, ALONG)
    packed = jnp.zeros((key_dim, heads * value_dim), F32)
    for head in range(heads):
        packed = packed + masked(cross[head * key_dim : (head + 1) * key_dim], head, value_dim)
    inject_ref[...] = packed.astype(BF16)


def inner_kernel(o_ref, v_ref, q_ref, k_ref, decay_ref, decay_t_ref, scores_t_ref, sum_ref, state_ref, query_ref, key_ref, value_ref, *, heads, key_dim, value_dim):
    o, v, q, k = o_ref[...], v_ref[...], q_ref[...], k_ref[...]
    growth = spread_heads(jnp.exp(sum_ref[...]), q.shape, key_dim)
    query = growth * dot(o, state_ref[...], ACROSS)
    key = jnp.zeros(k.shape, F32)
    value = jnp.zeros(v.shape, F32)
    for head in range(heads):
        o_head = masked(o, head, value_dim)
        prob = (dot(o_head, v, ACROSS) * decay_ref[head]).astype(BF16)
        prob_t = (dot(v, o_head, ACROSS) * decay_t_ref[head]).astype(BF16)
        query = query + dot(prob, masked(k, head, key_dim))
        key = key + dot(prob_t, masked(q, head, key_dim))
        value = value + dot(scores_t_ref[head], o_head)
    query_ref[...] = query.astype(BF16)
    key_ref[...] = key
    value_ref[...] = value


def outer_kernel(sp_ref, blocks_ref, sum_ref, k_ref, v_ref, key_in_ref, value_in_ref, *refs, heads, key_dim, value_dim):
    k, v = k_ref[...], v_ref[...]
    *arrived, key_ref, value_ref = refs
    state = jnp.zeros(arrived[0].shape, F32)
    here = sp_ref[0]
    for at, arrived_ref in enumerate(arrived):
        source = here ^ 1 if at == 0 else (here ^ (2 * at)) & ~1
        total = jnp.zeros((1, state.shape[1]), F32)
        for block in range(blocks_ref.shape[0]):
            between = (block > here) & (block < source)
            total = total + jnp.where(between, blocks_ref[block : block + 1, :], 0.0)
        state = state + arrived_ref[...].astype(F32) * jnp.where(source > here, jnp.exp(total), 0.0)
    state = blocks_on_diagonal(state, heads, value_dim).astype(BF16)
    sums = sum_ref[...]
    tail = jnp.exp(sums[sums.shape[0] - 1 :, :] - sums)
    key_ref[...] = (
        key_in_ref[...] + spread_heads(tail, k.shape, key_dim) * dot(v, state, ACROSS)
    ).astype(BF16)
    value_ref[...] = (
        value_in_ref[...] + spread_heads(tail, v.shape, value_dim) * dot(k, state)
    ).astype(BF16)


def weights_kernel(at_ref, gate_ref, up_ref, down_ref, mine_in, other_in, mine_down, other_down, arrivals, *, even, columns):
    hidden = gate_ref.shape[1]
    copies = []
    for low, (into, down) in enumerate(((mine_in, mine_down), (other_in, other_down))):
        for position, at in enumerate(even):
            source = pl.ds(pl.multiple_of((at_ref[0] ^ (at ^ low)) * columns, 128), columns)
            target = pl.ds(position * columns, columns)
            for from_ref, to_ref in (
                (gate_ref.at[source, :], into.at[target, pl.ds(0, hidden)]),
                (up_ref.at[source, :], into.at[target, pl.ds(hidden, hidden)]),
                (down_ref.at[:, source], down.at[:, target]),
            ):
                copies.append(pltpu.make_async_copy(from_ref, to_ref, arrivals.at[len(copies)]))
                copies[-1].start()
    for copy in copies:
        copy.wait()


def chosen(mine, other):
    return jnp.where(pl.program_id(1) == 0, mine[...], other[...])


def down_kernel(at_ref, *refs):
    acts, mine, other, out = refs[:CHUNKS], refs[CHUNKS : 2 * CHUNKS], refs[2 * CHUNKS : 3 * CHUNKS], refs[-1]
    total = sum([dot(act[...], chosen(m, o), ALONG) for act, m, o in zip(acts, mine, other)])
    out[...] = total.astype(BF16)


def into_kernel(at_ref, *refs):
    gates, ups, mine, other = [refs[n * CHUNKS : (n + 1) * CHUNKS] for n in range(4)]
    pieces = [chosen(m, o) for m, o in zip(mine, other)]
    for grads, out in ((gates, refs[-2]), (ups, refs[-1])):
        out[...] = sum([dot(p, g[...], ALONG) for p, g in zip(pieces, grads)]).astype(BF16)


def stream_kernel(at_ref, mine_ref, other_ref, stream_ref, send_ref, *, even, columns):
    _, half, out_columns = send_ref.shape
    per_piece = columns // out_columns
    row = pl.multiple_of((at_ref[0] & 1) * half, 16)
    for low, ref in enumerate((mine_ref, other_ref)):
        for position, at in enumerate(even):
            place = at_ref[0] ^ (at ^ low)
            span = pl.ds(position * columns, columns)
            stream_ref[:, pl.ds(pl.multiple_of(place * columns, 128), columns)] = ref[:, span]
            for b in range(per_piece):
                send_ref[place * per_piece + b] = ref[
                    pl.ds(row, half), pl.ds(position * columns + b * out_columns, out_columns)
                ]


def assemble_kernel(*refs):
    *pieces, rows_ref, grad_ref = refs
    columns = pieces[0].shape[1] // 2
    across = rows_ref.shape[1] // columns
    slots = pieces[0].shape[0]
    for n, piece in enumerate(pieces):
        block = pl.ds(n // across * slots, slots)
        span = pl.ds(n % across * columns, columns)
        rows_ref[block, span] = piece[:, :columns]
        grad_ref[block, span] = piece[:, columns:]


def shaped(shape, dtype):
    return jax.ShapeDtypeStruct(shape, dtype)


def call(kernel, out_shape, flops, *args, megabytes=12, **settings):
    return pl.pallas_call(
        functools.partial(kernel, **settings) if settings else kernel,
        in_specs=[
            pl.BlockSpec(memory_space=pltpu.SMEM if arg.dtype == jnp.int32 and arg.ndim == 1 else pltpu.VMEM)
            for arg in args
        ],
        out_specs=jax.tree.map(lambda _: pl.BlockSpec(memory_space=pltpu.VMEM), out_shape),
        out_shape=out_shape,
        compiler_params=pltpu.CompilerParams(vmem_limit_bytes=megabytes << 20),
        cost_estimate=pl.CostEstimate(flops=flops, bytes_accessed=1 << 20, transcendentals=0),
    )(*args)


def on_device(
    moe_input,
    out_grad,
    expert_ids,
    expert_weights,
    w_gate,
    w_up,
    w_down,
    out_proj,
    retained,
    queries,
    keys,
    values,
    log_decay,
    incoming_state,
):
    tokens_here, width = moe_input.shape
    sp_count = lax.axis_size("sp")
    tp_count = lax.axis_size("tp")
    sp_at = lax.axis_index("sp")
    tp_at = lax.axis_index("tp")
    tp_bits = powers(tp_count)
    far_bits = tp_bits[:0:-1]
    capacity = 5 * tokens_here // (2 * sp_count)
    slots = -(-capacity // 16) * 16
    slot_count = sp_count * slots
    columns = width // tp_count
    heads = log_decay.shape[1]
    key_width, value_width = queries.shape[1], values.shape[1]
    key_dim, value_dim = key_width // heads, value_width // heads
    hidden = w_gate.shape[2]

    hbm = pl.BlockSpec(memory_space=pltpu.HBM)
    vmem = pl.BlockSpec(memory_space=pltpu.VMEM)
    smem = pl.BlockSpec(memory_space=pltpu.SMEM)
    even = [0]
    for bit in far_bits:
        even = even + [at ^ bit for at in even]

    log_rows = log_decay.T
    if heads == 1:
        log_rows = jnp.pad(log_rows, ((0, 7), (0, 0)))
    square = (heads, tokens_here, tokens_here)
    sources = (
        expert_ids.T,
        expert_weights.T,
        moe_input,
        out_grad,
        log_rows,
        queries,
        keys,
        incoming_state[0],
        retained,
    )
    held = [shaped((tokens_here, columns) if n == 2 else x.shape, x.dtype) for n, x in enumerate(sources)]
    plain = pl.BlockSpec(memory_space=None)
    into = shaped((len(even) * columns, 2 * hidden), BF16)
    down = shaped((hidden, len(even) * columns), BF16)
    (
        *to_send,
        picker,
        decay,
        decay_t,
        scores_t,
        grown,
        running_total,
        incoming,
        wide,
    ) = pl.pallas_call(
        functools.partial(
            start_kernel, slots=slots, blocks=sp_count, heads=heads, key_dim=key_dim, value_dim=value_dim
        ),
        in_specs=[smem, smem] + [hbm] * len(sources),
        out_specs=[vmem] * sp_count + [plain] * 8,
        out_shape=[shaped((slots, 2 * columns), BF16)] * sp_count
        + [
            shaped((tokens_here, slot_count), BF16),
            shaped(square, F32),
            shaped(square, F32),
            shaped(square, BF16),
            shaped(queries.shape, BF16),
            shaped(log_decay.shape, F32),
            shaped((key_width, value_width), BF16),
            shaped((1, tokens_here + 16, value_width), BF16),
        ],
        scratch_shapes=[pltpu.VMEM(x.shape, x.dtype) for x in held] + [pltpu.SemaphoreType.DMA((len(held),))],
        compiler_params=pltpu.CompilerParams(vmem_limit_bytes=START_VMEM),
        cost_estimate=pl.CostEstimate(
            flops=4 * slot_count * tokens_here * columns, bytes_accessed=1 << 20, transcendentals=0
        ),
        name="start",
    )(tp_at.reshape(1), sp_at.reshape(1), *sources)

    def near(x):
        return swap(x, "tp", 1)

    def block_of(x, k):
        return x[k * slots : (k + 1) * slots]

    parts = [to_send[0]]
    for k in range(1, sp_count):
        parts.append(swap(to_send[k], "sp", k))

    def far_pieces(x):
        pieces = [x]
        for bit in far_bits:
            pieces = pieces + [swap(piece, "tp", bit) for piece in pieces]
        return pieces

    mine_in, other_in, mine_down, other_down = pl.pallas_call(
        functools.partial(weights_kernel, even=even, columns=columns),
        in_specs=[smem, hbm, hbm, hbm],
        out_specs=[vmem] * 4,
        out_shape=[into, into, down, down],
        scratch_shapes=[pltpu.SemaphoreType.DMA((3 * tp_count,))],
        compiler_params=pltpu.CompilerParams(vmem_limit_bytes=WEIGHTS_VMEM),
        cost_estimate=pl.CostEstimate(flops=1 << 30, bytes_accessed=1 << 20, transcendentals=0),
        name="weights",
    )(tp_at.reshape(1), w_gate[0], w_up[0], w_down[0])

    gathered = [far_pieces(x) for x in parts]
    per_chunk = sp_count // CHUNKS
    rows_mine, rows_other, grad_mine, grad_other = [], [], [], []
    for c in range(CHUNKS):
        of_chunk = [piece for k in range(c * per_chunk, (c + 1) * per_chunk) for piece in gathered[k]]
        joined = shaped((per_chunk * slots, len(even) * columns), BF16)
        whole = call(assemble_kernel, [joined, joined], 1 << 28, *of_chunk)
        rows_mine.append(whole[0])
        grad_mine.append(whole[1])
        rows_other.append(near(whole[0]))
        grad_other.append(near(whole[1]))

    acts, gate_grads, up_grads, returned = [], [], [], []
    for c in range(CHUNKS):
        both = dot(rows_mine[c], mine_in) + dot(rows_other[c], other_in)
        gate, up = both[:, :hidden], both[:, hidden:]
        sig = jax.nn.sigmoid(gate)
        swish = gate * sig
        acts.append((swish * up).astype(BF16))
        act_grad = dot(grad_mine[c], mine_down, ACROSS) + dot(grad_other[c], other_down, ACROSS)
        gate_grad = (act_grad * up * sig * (1.0 + gate * (1.0 - sig))).astype(BF16)
        up_grad = (act_grad * swish).astype(BF16)
        gate_grads.append(gate_grad)
        up_grads.append(up_grad)
        both_grad = jnp.concatenate([gate_grad, up_grad], axis=1)
        arrived = near(dot(both_grad, other_in, ACROSS).astype(BF16))
        sums = {}
        for position, at in reversed(list(enumerate(even))):
            span = slice(position * columns, (position + 1) * columns)
            sums[at] = dot(both_grad, mine_in[span], ACROSS) + arrived[:, span].astype(F32)
        for bit in tp_bits[1:]:
            sums = {
                at: sums[at] + swap(sums[at ^ bit].astype(BF16), "tp", bit).astype(F32)
                for at in sums
                if not at & bit
            }
        share = sums[0].astype(BF16)
        for k in range(per_chunk):
            block = block_of(share, k)
            at = c * per_chunk + k
            returned.append(swap(block, "sp", at) if at else block)

    places = jnp.asarray([at ^ low for at in even for low in (0, 1)], jnp.int32) ^ tp_at
    chunk_rows = per_chunk * slots
    narrow = pl.BlockSpec((chunk_rows, columns), lambda p, low, at: (0, p))
    fixed = pl.BlockSpec((chunk_rows, hidden), lambda p, low, at: (0, 0))
    by_row = pl.BlockSpec((columns, hidden), lambda p, low, at: (at[2 * p + low], 0))
    by_column = pl.BlockSpec((hidden, columns), lambda p, low, at: (0, at[2 * p + low]))

    def gradients(kernel, in_specs, out_specs, out_shape, *args):
        return pl.pallas_call(
            kernel,
            grid_spec=pltpu.PrefetchScalarGridSpec(
                num_scalar_prefetch=1, grid=(len(even), 2), in_specs=in_specs, out_specs=out_specs
            ),
            out_shape=out_shape,
            compiler_params=pltpu.CompilerParams(vmem_limit_bytes=16 << 20),
            cost_estimate=pl.CostEstimate(flops=1 << 32, bytes_accessed=1 << 20, transcendentals=0),
        )(places, *args)

    (down_grad,) = gradients(
        down_kernel,
        [fixed] * CHUNKS + [narrow] * (2 * CHUNKS),
        [by_column],
        [shaped((hidden, width), BF16)],
        *acts,
        *grad_mine,
        *grad_other,
    )
    gate_w_grad, up_w_grad = gradients(
        into_kernel,
        [fixed] * (2 * CHUNKS) + [narrow] * (2 * CHUNKS),
        [by_row, by_row],
        [shaped((width, hidden), BF16)] * 2,
        *gate_grads,
        *up_grads,
        *rows_mine,
        *rows_other,
    )

    token_grad = dot(picker, jnp.concatenate(returned, axis=0))
    stream_part = (out_grad.astype(F32) + token_grad).astype(BF16)
    stream_mine = jnp.concatenate(far_pieces(stream_part), axis=1)
    stream_other = near(stream_mine)
    half = tokens_here // 2
    out_columns = width // sp_count
    stream, columns_out = call(
        functools.partial(stream_kernel, even=even, columns=columns),
        [shaped((tokens_here, width), BF16), shaped((sp_count, half, out_columns), BF16)],
        1 << 28,
        tp_at.reshape(1),
        stream_mine,
        stream_other,
    )

    sp_bits = powers(sp_count)
    turn = sp_bits[1:] + sp_bits[:1]
    for bit in turn[:-1]:
        wide = jnp.concatenate([wide, swap(wide, "sp", bit)], axis=0)
    last = swap(wide, "sp", turn[-1])

    halves = shaped((sp_count * half, value_width), BF16)
    own_rows, other_rows, block_sums = call(
        functools.partial(order_kernel, turn=tuple(turn)),
        [halves, halves, shaped((sp_count, value_width), F32)],
        1 << 28,
        tp_at.reshape(1),
        sp_at.reshape(1),
        wide,
        last,
    )

    got_half = lax.all_to_all(columns_out, "sp", split_axis=0, concat_axis=0, tiled=True)
    other_half = near(got_half)
    own_cols = got_half.reshape(-1, out_columns)
    other_cols = other_half.reshape(-1, out_columns)
    own_part = dot(own_cols, own_rows, ALONG)
    out_proj_grad = own_part + dot(other_cols, other_rows, ALONG)

    sizes = dict(heads=heads, key_dim=key_dim, value_dim=value_dim)
    o, added = call(
        inject_kernel,
        [
            shaped((tokens_here, value_width), BF16),
            shaped((key_dim, value_width), BF16),
        ],
        1 << 30,
        stream,
        out_proj,
        grown,
        **sizes,
    )
    partner = swap(added, "sp", 1)
    pair = call(pair_kernel, shaped(added.shape, BF16), 1 << 26, sp_at.reshape(1), block_sums, added, partner)
    arrived = [partner]
    for k in range(2, sp_count, 2):
        arrived.append(swap(pair, "sp", k))

    query_grad, key_inner, value_inner = call(
        inner_kernel,
        [shaped(queries.shape, BF16), shaped(keys.shape, F32), shaped(values.shape, F32)],
        1 << 32,
        o,
        values,
        queries,
        keys,
        decay,
        decay_t,
        scores_t,
        running_total,
        incoming,
        **sizes,
    )

    key_grad, value_grad = call(
        outer_kernel,
        [shaped(keys.shape, BF16), shaped(values.shape, BF16)],
        1 << 30,
        sp_at.reshape(1),
        block_sums,
        running_total,
        keys,
        values,
        key_inner,
        value_inner,
        *arrived,
        **sizes,
    )
    return (
        gate_w_grad[None],
        up_w_grad[None],
        down_grad[None],
        out_proj_grad,
        query_grad,
        key_grad,
        value_grad,
    )


def solution(mesh):
    placed = (
        P("sp", None),
        P("sp", "tp"),
        P("sp", None),
        P("sp", None),
        P("sp", None, "tp"),
        P("sp", None, "tp"),
        P("sp", "tp", None),
        P("tp", None),
        P("sp", "tp"),
        P("sp", "tp"),
        P("sp", "tp"),
        P("sp", "tp"),
        P("sp", "tp"),
        P("sp", "tp", None, None),
    )

    return jax.shard_map(
        on_device,
        mesh=mesh,
        in_specs=placed,
        out_specs=(
            P("sp", None, "tp"),
            P("sp", None, "tp"),
            P("sp", "tp", None),
            P("sp", "tp"),
            P("sp", "tp"),
            P("sp", "tp"),
            P("sp", "tp"),
        ),
        check_vma=False,
    )
```

```python
import functools

import jax
import jax.numpy as jnp
from jax import lax
from jax.experimental import pallas as pl
from jax.experimental.pallas import tpu as pltpu
from jax.sharding import PartitionSpec as P


F32 = jnp.float32
BF16 = jnp.bfloat16
ACROSS = (((1,), (1,)), ((), ()))
ALONG = (((0,), (0,)), ((), ()))
CHUNKS = 2
START_VMEM = 60 << 20
WEIGHTS_VMEM = 46 << 20
INNER_MB = 58


def swap(x, axis, offset):
    count = lax.axis_size(axis)
    return lax.ppermute(x, axis, [(d, d ^ offset) for d in range(count)])


def powers(count):
    bits = []
    bit = 1
    while bit < count:
        bits.append(bit)
        bit *= 2
    return bits


def dot(a, b, dims=(((1,), (0,)), ((), ()))):
    return lax.dot_general(a, b, dims, preferred_element_type=F32)


def lanes(shape, head, per_head):
    lane = lax.broadcasted_iota(jnp.int32, shape, 1)
    return (lane >= head * per_head) & (lane < (head + 1) * per_head)


def spread_heads(columns, shape, per_head):
    out = jnp.zeros(shape, F32)
    for head in range(shape[1] // per_head):
        out = jnp.where(lanes(shape, head, per_head), columns[:, head : head + 1], out)
    return out


def masked(x, head, per_head):
    return jnp.where(lanes(x.shape, head, per_head), x, jnp.zeros_like(x))


def blocks_on_diagonal(packed, heads, value_dim):
    return jnp.concatenate([masked(packed, head, value_dim) for head in range(heads)], axis=0)


def start_kernel(tp_ref, sp_ref, *refs, slots, blocks, heads, key_dim, value_dim):
    sources, outs, scratch, arrivals = refs[:8], refs[8 : 14 + blocks], refs[14 + blocks : -1], refs[-1]
    send_refs, outs = outs[:blocks], outs[blocks:]
    columns = scratch[3].shape[1]
    start = pl.multiple_of(tp_ref[0] * columns, 128)
    copies = [
        pltpu.make_async_copy(
            source.at[:, pl.ds(start, columns)] if n == 2 else source, target, arrivals.at[n]
        )
        for n, (source, target) in enumerate(zip(sources, scratch))
    ]
    for copy in copies:
        copy.start()
    pick_part(copies, sp_ref, *scratch[:4], send_refs, outs[0], slots=slots, blocks=blocks)
    for copy in copies[4:]:
        copy.wait()
    prepare_part(*scratch[4:], *outs[1:], heads=heads, key_dim=key_dim, value_dim=value_dim)


def pick_part(copies, sp_ref, ids_ref, weights_ref, rows_ref, grad_ref, send_refs, pick_ref, *, slots, blocks):
    columns = grad_ref.shape[1]
    copies[0].wait()
    tokens = ids_ref.shape[1]
    total = slots * blocks
    first, second = ids_ref[0:1, :], ids_ref[1:2, :]
    expert = lax.broadcasted_iota(jnp.int32, (-(-blocks // 16) * 16, tokens), 0)
    one, two = expert == first, expert == second
    both = jnp.where(one | two, 1.0, 0.0).astype(BF16)
    row = lax.broadcasted_iota(jnp.int32, (tokens, tokens), 0)
    col = lax.broadcasted_iota(jnp.int32, (tokens, tokens), 1)
    count = dot(both, jnp.where(row < col, 1.0, 0.0).astype(BF16))
    rank_one = jnp.sum(jnp.where(one, count, 0.0), axis=0, keepdims=True)
    rank_two = jnp.sum(jnp.where(two, count, 0.0), axis=0, keepdims=True)

    slot_one = (first ^ sp_ref[0]) * slots + rank_one.astype(jnp.int32)
    slot_two = (second ^ sp_ref[0]) * slots + rank_two.astype(jnp.int32)
    position = lax.broadcasted_iota(jnp.int32, (total, tokens), 0)
    hit_one, hit_two = position == slot_one, position == slot_two
    pick = jnp.where(hit_one | hit_two, 1.0, 0.0).astype(BF16)
    copies[1].wait()
    weight = jnp.sum(
        jnp.where(hit_one, weights_ref[0:1, :], 0.0) + jnp.where(hit_two, weights_ref[1:2, :], 0.0),
        axis=1,
        keepdims=True,
    )
    copies[2].wait()
    rows = dot(pick, rows_ref[...]).astype(BF16)
    copies[3].wait()
    grad = (dot(pick, grad_ref[...]) * weight).astype(BF16)
    for k in range(blocks):
        send_refs[k][:, :columns] = rows[k * slots : (k + 1) * slots]
        send_refs[k][:, columns:] = grad[k * slots : (k + 1) * slots]
    diagonal = row == col

    def as_column(line):
        return jnp.sum(jnp.where(diagonal, line, jnp.zeros_like(line)), axis=1, keepdims=True)

    place = lax.broadcasted_iota(jnp.int32, (tokens, total), 1)
    found = (place == as_column(slot_one)) | (place == as_column(slot_two))
    pick_ref[...] = jnp.where(found, 1.0, 0.0).astype(BF16)


def three_terms(x):
    high = x.astype(BF16)
    rest = x - high.astype(F32)
    middle = rest.astype(BF16)
    return high, middle, (rest - middle.astype(F32)).astype(BF16)


def prepare_part(log_ref, q_ref, state_ref, kept_ref, qe_ref, sum_ref, flat_ref, incoming_ref, wide_ref, *, heads, key_dim, value_dim):
    tokens = q_ref.shape[0]
    row = lax.broadcasted_iota(jnp.int32, (tokens, tokens), 0)
    col = lax.broadcasted_iota(jnp.int32, (tokens, tokens), 1)
    below = jnp.where(col <= row, 1.0, 0.0).astype(BF16)
    terms = three_terms(log_ref[...])
    sums = sum([dot(below, term, ACROSS) for term in terms])
    sum_ref[...] = sums[:, :heads]
    flat_ref[...] = sum([dot(term, below, ACROSS) for term in terms])[:heads]
    q = q_ref[...]
    qe_ref[...] = (q.astype(F32) * spread_heads(jnp.exp(sums), q.shape, key_dim)).astype(BF16)
    width = heads * value_dim
    from_lane = lax.broadcasted_iota(jnp.int32, (value_dim, width), 0)
    to_lane = lax.broadcasted_iota(jnp.int32, (value_dim, width), 1)
    for head in range(heads):
        put = jnp.where(to_lane == from_lane + head * value_dim, 1.0, 0.0).astype(BF16)
        incoming_ref[head * key_dim : (head + 1) * key_dim, :] = dot(
            state_ref[head].astype(BF16), put
        ).astype(BF16)
    last = spread_heads(sums[tokens - 8 : tokens], (8, width), value_dim)[7:8]
    high, middle, low = three_terms(last)
    line = lax.broadcasted_iota(jnp.int32, (16, width), 0)
    extra = jnp.where(line == 0, high.astype(F32), 0.0)
    extra = jnp.where(line == 1, middle.astype(F32), extra)
    extra = jnp.where(line == 2, low.astype(F32), extra)
    extra = extra.astype(BF16)
    kept = kept_ref[...]
    for block in range(wide_ref.shape[0]):
        wide_ref[block, :tokens, :] = kept
        wide_ref[block, tokens:, :] = extra


def order_kernel(tp_ref, sp_ref, wide_ref, last_ref, own_ref, other_ref, sums_ref):
    kept, rows, _ = wide_ref.shape
    half = (rows - 16) // 2
    own = pl.multiple_of((tp_ref[0] & 1) * half, 16)
    for position in range(2 * kept):
        offset = 2 * position if position < kept else 2 * (position - kept) + 1
        ref, at = (wide_ref, position) if position < kept else (last_ref, position - kept)
        block = sp_ref[0] ^ offset
        target = pl.ds(pl.multiple_of(block * half, 16), half)
        own_ref[target, :] = ref[at, pl.ds(own, half), :]
        other_ref[target, :] = ref[at, pl.ds(half - own, half), :]
        tail = ref[at, 2 * half :, :].astype(F32)
        sums_ref[pl.ds(block, 1), :] = tail[0:1] + tail[1:2] + tail[2:3]


def pair_kernel(sp_ref, sums_ref, added_ref, partner_ref, pair_ref):
    odd = (sp_ref[0] & 1) == 1
    added, partner = added_ref[...].astype(F32), partner_ref[...].astype(F32)
    first, second = jnp.where(odd, partner, added), jnp.where(odd, added, partner)
    decay = jnp.exp(sums_ref[pl.ds(sp_ref[0] & ~1, 1), :])
    pair_ref[...] = (first + decay * second).astype(BF16)


def inner_kernel(o_ref, v_ref, q_ref, k_ref, sum_ref, flat_ref, state_ref, query_ref, key_ref, value_ref, *, heads, key_dim, value_dim):
    o, v, q, k = o_ref[...], v_ref[...], q_ref[...], k_ref[...]
    tokens = q.shape[0]
    row = lax.broadcasted_iota(jnp.int32, (tokens, tokens), 0)
    col = lax.broadcasted_iota(jnp.int32, (tokens, tokens), 1)
    sums = sum_ref[...]
    query = spread_heads(jnp.exp(sums), q.shape, key_dim) * dot(o, state_ref[...], ACROSS)
    key = jnp.zeros(k.shape, F32)
    value = jnp.zeros(v.shape, F32)
    for head in range(heads):
        down, flat = sums[:, head : head + 1], flat_ref[head : head + 1, :]
        decay = jnp.where(row >= col, jnp.exp(jnp.minimum(down - flat, 0.0)), 0.0)
        decay_t = jnp.where(col >= row, jnp.exp(jnp.minimum(flat - down, 0.0)), 0.0)
        o_head = masked(o, head, value_dim)
        k_head = masked(k, head, key_dim)
        prob = (dot(o_head, v, ACROSS) * decay).astype(BF16)
        prob_t = (dot(v, o_head, ACROSS) * decay_t).astype(BF16)
        scores_t = (dot(k_head, q, ACROSS) * decay_t).astype(BF16)
        query = query + dot(prob, k_head)
        key = key + dot(prob_t, masked(q, head, key_dim))
        value = value + dot(scores_t, o_head)
    query_ref[...] = query.astype(BF16)
    key_ref[...] = key
    value_ref[...] = value


def outer_kernel(sp_ref, blocks_ref, sum_ref, k_ref, v_ref, key_in_ref, value_in_ref, *refs, heads, key_dim, value_dim):
    k, v = k_ref[...], v_ref[...]
    *arrived, key_ref, value_ref = refs
    state = jnp.zeros(arrived[0].shape, F32)
    here = sp_ref[0]
    for at, arrived_ref in enumerate(arrived):
        source = here ^ 1 if at == 0 else (here ^ (2 * at)) & ~1
        total = jnp.zeros((1, state.shape[1]), F32)
        for block in range(blocks_ref.shape[0]):
            between = (block > here) & (block < source)
            total = total + jnp.where(between, blocks_ref[block : block + 1, :], 0.0)
        state = state + arrived_ref[...].astype(F32) * jnp.where(source > here, jnp.exp(total), 0.0)
    state = blocks_on_diagonal(state, heads, value_dim).astype(BF16)
    sums = sum_ref[...]
    tail = jnp.exp(sums[sums.shape[0] - 1 :, :] - sums)
    key_ref[...] = (
        key_in_ref[...] + spread_heads(tail, k.shape, key_dim) * dot(v, state, ACROSS)
    ).astype(BF16)
    value_ref[...] = (
        value_in_ref[...] + spread_heads(tail, v.shape, value_dim) * dot(k, state)
    ).astype(BF16)


def weights_kernel(at_ref, gate_ref, up_ref, down_ref, mine_in, other_in, mine_down, other_down, arrivals, *, even, columns):
    hidden = gate_ref.shape[1]
    copies = []
    for low, (into, down) in enumerate(((mine_in, mine_down), (other_in, other_down))):
        for position, at in enumerate(even):
            source = pl.ds(pl.multiple_of((at_ref[0] ^ (at ^ low)) * columns, 128), columns)
            target = pl.ds(position * columns, columns)
            for from_ref, to_ref in (
                (gate_ref.at[source, :], into.at[target, pl.ds(0, hidden)]),
                (up_ref.at[source, :], into.at[target, pl.ds(hidden, hidden)]),
                (down_ref.at[:, source], down.at[:, target]),
            ):
                copies.append(pltpu.make_async_copy(from_ref, to_ref, arrivals.at[len(copies)]))
                copies[-1].start()
    for copy in copies:
        copy.wait()


def chosen(mine, other):
    return jnp.where(pl.program_id(1) == 0, mine[...], other[...])


def down_kernel(at_ref, *refs):
    acts, mine, other, out = refs[:CHUNKS], refs[CHUNKS : 2 * CHUNKS], refs[2 * CHUNKS : 3 * CHUNKS], refs[-1]
    total = sum([dot(act[...], chosen(m, o), ALONG) for act, m, o in zip(acts, mine, other)])
    out[...] = total.astype(BF16)


def into_kernel(at_ref, *refs):
    gates, ups, mine, other = [refs[n * CHUNKS : (n + 1) * CHUNKS] for n in range(4)]
    pieces = [chosen(m, o) for m, o in zip(mine, other)]
    for grads, out in ((gates, refs[-2]), (ups, refs[-1])):
        out[...] = sum([dot(p, g[...], ALONG) for p, g in zip(pieces, grads)]).astype(BF16)


def combine_kernel(pick_ref, grad_ref, *refs):
    *pieces, stream_ref, joined = refs
    slots = pieces[0].shape[0]
    for k, piece in enumerate(pieces):
        joined[k * slots : (k + 1) * slots, :] = piece[...]
    total = grad_ref[...].astype(F32) + dot(pick_ref[...], joined[...])
    stream_ref[...] = total.astype(BF16)


def project_kernel(columns_ref, rows_ref, *refs):
    total = dot(columns_ref[...], rows_ref[...], ALONG)
    if len(refs) == 2:
        total = total + refs[0][...]
    refs[-1][...] = total


def stream_kernel(at_ref, mine_ref, other_ref, proj_ref, qe_ref, send_ref, o_ref, inject_ref, stream_ref, *, even, columns, heads, key_dim, value_dim):
    _, half, out_columns = send_ref.shape
    per_piece = columns // out_columns
    row = pl.multiple_of((at_ref[0] & 1) * half, 16)
    for low, ref in enumerate((mine_ref, other_ref)):
        for position, at in enumerate(even):
            place = at_ref[0] ^ (at ^ low)
            span = pl.ds(position * columns, columns)
            stream_ref[:, pl.ds(pl.multiple_of(place * columns, 128), columns)] = ref[:, span]
            for b in range(per_piece):
                send_ref[place * per_piece + b] = ref[
                    pl.ds(row, half), pl.ds(position * columns + b * out_columns, out_columns)
                ]
    o = dot(stream_ref[...], proj_ref[...], ACROSS).astype(BF16)
    o_ref[...] = o
    cross = dot(qe_ref[...], o, ALONG)
    packed = jnp.zeros((key_dim, heads * value_dim), F32)
    for head in range(heads):
        packed = packed + masked(cross[head * key_dim : (head + 1) * key_dim], head, value_dim)
    inject_ref[...] = packed.astype(BF16)


def assemble_kernel(*refs):
    *pieces, rows_ref, grad_ref = refs
    columns = pieces[0].shape[1] // 2
    across = rows_ref.shape[1] // columns
    slots = pieces[0].shape[0]
    for n, piece in enumerate(pieces):
        block = pl.ds(n // across * slots, slots)
        span = pl.ds(n % across * columns, columns)
        rows_ref[block, span] = piece[:, :columns]
        grad_ref[block, span] = piece[:, columns:]


def shaped(shape, dtype):
    return jax.ShapeDtypeStruct(shape, dtype)


def call(kernel, out_shape, flops, *args, megabytes=12, scratch=(), plain=False, plain_outs=(), **settings):
    space = None if plain else pltpu.VMEM
    out_space = pltpu.VMEM
    shapes, tree = jax.tree.flatten(out_shape)
    outs = [pl.BlockSpec(memory_space=None if n in plain_outs else out_space) for n in range(len(shapes))]
    return pl.pallas_call(
        functools.partial(kernel, **settings) if settings else kernel,
        in_specs=[
            pl.BlockSpec(memory_space=pltpu.SMEM if arg.dtype == jnp.int32 and arg.ndim == 1 else space)
            for arg in args
        ],
        out_specs=jax.tree.unflatten(tree, outs),
        out_shape=out_shape,
        scratch_shapes=scratch,
        compiler_params=pltpu.CompilerParams(vmem_limit_bytes=megabytes << 20),
        cost_estimate=pl.CostEstimate(flops=flops, bytes_accessed=1 << 20, transcendentals=0),
    )(*args)


def on_device(
    moe_input,
    out_grad,
    expert_ids,
    expert_weights,
    w_gate,
    w_up,
    w_down,
    out_proj,
    retained,
    queries,
    keys,
    values,
    log_decay,
    incoming_state,
):
    tokens_here, width = moe_input.shape
    sp_count = lax.axis_size("sp")
    tp_count = lax.axis_size("tp")
    sp_at = lax.axis_index("sp")
    tp_at = lax.axis_index("tp")
    tp_bits = powers(tp_count)
    far_bits = tp_bits[:0:-1]
    capacity = 5 * tokens_here // (2 * sp_count)
    slots = -(-capacity // 16) * 16
    slot_count = sp_count * slots
    columns = width // tp_count
    heads = log_decay.shape[1]
    key_width, value_width = queries.shape[1], values.shape[1]
    key_dim, value_dim = key_width // heads, value_width // heads
    hidden = w_gate.shape[2]

    hbm = pl.BlockSpec(memory_space=pltpu.HBM)
    vmem = pl.BlockSpec(memory_space=pltpu.VMEM)
    smem = pl.BlockSpec(memory_space=pltpu.SMEM)
    even = [0]
    for bit in far_bits:
        even = even + [at ^ bit for at in even]

    log_rows = log_decay.T
    if heads == 1:
        log_rows = jnp.pad(log_rows, ((0, 7), (0, 0)))
    sources = (
        expert_ids.T,
        expert_weights.T,
        moe_input,
        out_grad,
        log_rows,
        queries,
        incoming_state[0],
        retained,
    )
    held = [shaped((tokens_here, columns) if n == 2 else x.shape, x.dtype) for n, x in enumerate(sources)]
    plain = pl.BlockSpec(memory_space=None)
    into = shaped((len(even) * columns, 2 * hidden), BF16)
    down = shaped((hidden, len(even) * columns), BF16)
    (
        *to_send,
        picker,
        grown,
        running_total,
        flat_total,
        incoming,
        wide,
    ) = pl.pallas_call(
        functools.partial(
            start_kernel, slots=slots, blocks=sp_count, heads=heads, key_dim=key_dim, value_dim=value_dim
        ),
        in_specs=[smem, smem] + [hbm] * len(sources),
        out_specs=[vmem] * sp_count + [plain] * 6,
        out_shape=[shaped((slots, 2 * columns), BF16)] * sp_count
        + [
            shaped((tokens_here, slot_count), BF16),
            shaped(queries.shape, BF16),
            shaped(log_decay.shape, F32),
            shaped(log_decay.shape[::-1], F32),
            shaped((key_width, value_width), BF16),
            shaped((1, tokens_here + 16, value_width), BF16),
        ],
        scratch_shapes=[pltpu.VMEM(x.shape, x.dtype) for x in held] + [pltpu.SemaphoreType.DMA((len(held),))],
        compiler_params=pltpu.CompilerParams(vmem_limit_bytes=START_VMEM),
        cost_estimate=pl.CostEstimate(
            flops=4 * slot_count * tokens_here * columns, bytes_accessed=1 << 20, transcendentals=0
        ),
        name="start",
    )(tp_at.reshape(1), sp_at.reshape(1), *sources)

    def near(x):
        return swap(x, "tp", 1)

    def block_of(x, k):
        return x[k * slots : (k + 1) * slots]

    parts = [to_send[0]]
    for k in range(1, sp_count):
        parts.append(swap(to_send[k], "sp", k))

    def far_pieces(x):
        pieces = [x]
        for bit in far_bits:
            pieces = pieces + [swap(piece, "tp", bit) for piece in pieces]
        return pieces

    mine_in, other_in, mine_down, other_down = pl.pallas_call(
        functools.partial(weights_kernel, even=even, columns=columns),
        in_specs=[smem, hbm, hbm, hbm],
        out_specs=[vmem] * 4,
        out_shape=[into, into, down, down],
        scratch_shapes=[pltpu.SemaphoreType.DMA((3 * tp_count,))],
        compiler_params=pltpu.CompilerParams(vmem_limit_bytes=WEIGHTS_VMEM),
        cost_estimate=pl.CostEstimate(flops=1 << 30, bytes_accessed=1 << 20, transcendentals=0),
        name="weights",
    )(tp_at.reshape(1), w_gate[0], w_up[0], w_down[0])

    gathered = [far_pieces(x) for x in parts]
    per_chunk = sp_count // CHUNKS
    rows_mine, rows_other, grad_mine, grad_other = [], [], [], []
    for c in range(CHUNKS):
        of_chunk = [piece for k in range(c * per_chunk, (c + 1) * per_chunk) for piece in gathered[k]]
        joined = shaped((per_chunk * slots, len(even) * columns), BF16)
        whole = call(assemble_kernel, [joined, joined], 1 << 28, *of_chunk)
        rows_mine.append(whole[0])
        grad_mine.append(whole[1])
        rows_other.append(near(whole[0]))
        grad_other.append(near(whole[1]))

    acts, gate_grads, up_grads, returned = [], [], [], []
    for c in range(CHUNKS):
        both = dot(rows_mine[c], mine_in) + dot(rows_other[c], other_in)
        gate, up = both[:, :hidden], both[:, hidden:]
        sig = jax.nn.sigmoid(gate)
        swish = gate * sig
        acts.append((swish * up).astype(BF16))
        act_grad = dot(grad_mine[c], mine_down, ACROSS) + dot(grad_other[c], other_down, ACROSS)
        gate_grad = (act_grad * up * sig * (1.0 + gate * (1.0 - sig))).astype(BF16)
        up_grad = (act_grad * swish).astype(BF16)
        gate_grads.append(gate_grad)
        up_grads.append(up_grad)
        both_grad = jnp.concatenate([gate_grad, up_grad], axis=1)
        arrived = near(dot(both_grad, other_in, ACROSS).astype(BF16))
        sums = {}
        for position, at in reversed(list(enumerate(even))):
            span = slice(position * columns, (position + 1) * columns)
            sums[at] = dot(both_grad, mine_in[span], ACROSS) + arrived[:, span].astype(F32)
        for bit in tp_bits[1:]:
            sums = {
                at: sums[at] + swap(sums[at ^ bit].astype(BF16), "tp", bit).astype(F32)
                for at in sums
                if not at & bit
            }
        share = sums[0].astype(BF16)
        for k in range(per_chunk):
            block = block_of(share, k)
            at = c * per_chunk + k
            returned.append(swap(block, "sp", at) if at else block)

    places = jnp.asarray([at ^ low for at in even for low in (0, 1)], jnp.int32) ^ tp_at
    chunk_rows = per_chunk * slots
    narrow = pl.BlockSpec((chunk_rows, columns), lambda p, low, at: (0, p))
    fixed = pl.BlockSpec((chunk_rows, hidden), lambda p, low, at: (0, 0))
    by_row = pl.BlockSpec((columns, hidden), lambda p, low, at: (at[2 * p + low], 0))
    by_column = pl.BlockSpec((hidden, columns), lambda p, low, at: (0, at[2 * p + low]))

    def gradients(kernel, in_specs, out_specs, out_shape, *args):
        return pl.pallas_call(
            kernel,
            grid_spec=pltpu.PrefetchScalarGridSpec(
                num_scalar_prefetch=1, grid=(len(even), 2), in_specs=in_specs, out_specs=out_specs
            ),
            out_shape=out_shape,
            compiler_params=pltpu.CompilerParams(vmem_limit_bytes=16 << 20),
            cost_estimate=pl.CostEstimate(flops=1 << 32, bytes_accessed=1 << 20, transcendentals=0),
        )(places, *args)

    (down_grad,) = gradients(
        down_kernel,
        [fixed] * CHUNKS + [narrow] * (2 * CHUNKS),
        [by_column],
        [shaped((hidden, width), BF16)],
        *acts,
        *grad_mine,
        *grad_other,
    )
    gate_w_grad, up_w_grad = gradients(
        into_kernel,
        [fixed] * (2 * CHUNKS) + [narrow] * (2 * CHUNKS),
        [by_row, by_row],
        [shaped((width, hidden), BF16)] * 2,
        *gate_grads,
        *up_grads,
        *rows_mine,
        *rows_other,
    )

    stream_part = call(
        combine_kernel, shaped(out_grad.shape, BF16), 1 << 27, picker, out_grad, *returned,
        scratch=[pltpu.VMEM((slot_count, columns), BF16)],
    )
    stream_mine = jnp.concatenate(far_pieces(stream_part), axis=1)
    stream_other = near(stream_mine)
    half = tokens_here // 2
    out_columns = width // sp_count
    sizes = dict(heads=heads, key_dim=key_dim, value_dim=value_dim)
    columns_out, o, added = call(
        functools.partial(stream_kernel, even=even, columns=columns),
        [
            shaped((sp_count, half, out_columns), BF16),
            shaped((tokens_here, value_width), BF16),
            shaped((key_dim, value_width), BF16),
        ],
        1 << 28,
        tp_at.reshape(1),
        stream_mine,
        stream_other,
        out_proj,
        grown,
        scratch=[pltpu.VMEM((tokens_here, width), BF16)],
        plain_outs=(1, 2),
        **sizes,
    )

    kept = [wide]
    for k in range(2, sp_count, 2):
        kept.append(swap(wide, "sp", k))
    near_kept = jnp.concatenate(kept, axis=0)
    far_kept = swap(near_kept, "sp", 1)

    halves = shaped((sp_count * half, value_width), BF16)
    own_rows, other_rows, block_sums = call(
        order_kernel,
        [halves, halves, shaped((sp_count, value_width), F32)],
        1 << 28,
        tp_at.reshape(1),
        sp_at.reshape(1),
        near_kept,
        far_kept,
    )

    got_half = lax.all_to_all(columns_out, "sp", split_axis=0, concat_axis=0, tiled=True)
    other_half = near(got_half)
    own_cols = got_half.reshape(-1, out_columns)
    other_cols = other_half.reshape(-1, out_columns)
    product = shaped((out_columns, value_width), F32)
    own_part = call(project_kernel, product, 1 << 28, own_cols, own_rows)
    out_proj_grad = call(project_kernel, product, 1 << 28, other_cols, other_rows, own_part)

    partner = swap(added, "sp", 1)
    pair = call(pair_kernel, shaped(added.shape, BF16), 1 << 26, sp_at.reshape(1), block_sums, added, partner)
    arrived = [partner]
    for k in range(2, sp_count, 2):
        arrived.append(swap(pair, "sp", k))

    query_grad, key_inner, value_inner = call(
        inner_kernel,
        [shaped(queries.shape, BF16), shaped(keys.shape, F32), shaped(values.shape, F32)],
        1 << 32,
        o,
        values,
        queries,
        keys,
        running_total,
        flat_total,
        incoming,
        megabytes=INNER_MB,
        plain=True,
        **sizes,
    )

    key_grad, value_grad = call(
        outer_kernel,
        [shaped(keys.shape, BF16), shaped(values.shape, BF16)],
        1 << 30,
        sp_at.reshape(1),
        block_sums,
        running_total,
        keys,
        values,
        key_inner,
        value_inner,
        *arrived,
        **sizes,
    )
    return (
        gate_w_grad[None],
        up_w_grad[None],
        down_grad[None],
        out_proj_grad,
        query_grad,
        key_grad,
        value_grad,
    )


def solution(mesh):
    placed = (
        P("sp", None),
        P("sp", "tp"),
        P("sp", None),
        P("sp", None),
        P("sp", None, "tp"),
        P("sp", None, "tp"),
        P("sp", "tp", None),
        P("tp", None),
        P("sp", "tp"),
        P("sp", "tp"),
        P("sp", "tp"),
        P("sp", "tp"),
        P("sp", "tp"),
        P("sp", "tp", None, None),
    )

    return jax.shard_map(
        on_device,
        mesh=mesh,
        in_specs=placed,
        out_specs=(
            P("sp", None, "tp"),
            P("sp", None, "tp"),
            P("sp", "tp", None),
            P("sp", "tp"),
            P("sp", "tp"),
            P("sp", "tp"),
            P("sp", "tp"),
        ),
        check_vma=False,
    )
```
